32 devices in a mesh: fs: 4 (over z), rep: 2 (over y), tp: 4 (over x, core).
Axes of the slice: x: 2, y: 2, z: 4, core: 2. Of those that a mesh axis runs over, the one named last changes fastest.
Arguments:
- saved_input: bfloat16 [5120, 3072], P(('fs', 'rep')), may hold values from -6 to 6
- key_cotangent: bfloat16 [5120, 1024], P(('fs', 'rep'), 'tp'), may hold values from -0.0625 to 0.0625
- value_cotangent: bfloat16 [5120, 2048], P(('fs', 'rep'), 'tp'), may hold values from -0.0625 to 0.0625
- key_factor: bfloat16 [3072, 256], replicated, may hold values from -0.375 to 0.375
- value_factor: bfloat16 [3072, 256], replicated, may hold values from -0.375 to 0.375
- key_weight: float32 [3072, 1024], P(('fs', 'rep'), 'tp'), may hold values from -0.109375 to 0.109375
- value_weight: float32 [3072, 2048], P(('fs', 'rep'), 'tp'), may hold values from -0.109375 to 0.109375
- key_first: float32 [256, 1024], P(None, 'tp'), as said below
- key_second: float32 [256, 1024], P(None, 'tp'), may hold values from 0.05 to 1
- value_first: float32 [256, 2048], P(None, 'tp'), as said below
- value_second: float32 [256, 2048], P(None, 'tp'), may hold values from 0.05 to 1
Outputs:
- key_weight_new: float32 [3072, 1024], P(('fs', 'rep'), 'tp')
- value_weight_new: float32 [3072, 2048], P(('fs', 'rep'), 'tp')
- key_first_new: float32 [256, 1024], P(None, 'tp')
- key_second_new: float32 [256, 1024], P(None, 'tp')
- value_first_new: float32 [256, 2048], P(None, 'tp')
- value_second_new: float32 [256, 2048], P(None, 'tp')
- key_step: float32 [3072, 1024], P(('fs', 'rep'), 'tp')
- value_step: float32 [3072, 2048], P(('fs', 'rep'), 'tp')
- key_copy: bfloat16 [3072, 1024], P(None, 'tp')
- value_copy: bfloat16 [3072, 2048], P(None, 'tp')
The draws below stay inside these ranges and needn't reach their ends.
Inputs may be any that keep to these rules, and one draw needn't show every extreme that they name: `key_first`: real-valued moments whose scale differs from head to head. `value_first`: real-valued moments whose scale differs from head to head.
All inputs are finite; a program needn't handle non-finite values.
Results may differ from the reference program's by a relative error of at most 0.004.
Values may be sent and summed in bfloat16 or wider, within the bound.
No kernel may reach another device: no remote copies, remote signals or barrier semaphores. Data moves between devices by JAX's collectives and lax.ppermute only.
A program may use at most 64 MiB of HBM per device.

```python
import math
import jax
import jax.numpy as jnp
from jax import lax

D = 3072
HEADS = 8
HK = 128
HV = 256
DK = 1024
DV = 2048
RK = 256
RV = 256
TOKENS = 5120


def head_scaled(key, row_count, head_count, head_width):
    scale_key, value_key = jax.random.split(key)
    spread = jnp.exp(jax.random.uniform(scale_key, (head_count,), jnp.float32, -1.4, 1.4))
    entries = jax.random.normal(value_key, (row_count, head_count, head_width), jnp.float32)
    return (entries * spread[None, :, None]).reshape(row_count, head_count * head_width)


def draw_key_first(key, part):
    return head_scaled(jax.random.fold_in(key, 3), RK, HEADS, HK)


def draw_value_first(key, part):
    return head_scaled(jax.random.fold_in(key, 7), RV, HEADS, HV)


def spiked(values, key, source, target, shards_of, factor):
    owner, partner = [(jnp.arange(values.shape[position]) // (values.shape[position] // shards_of)).reshape([-1 if axis == position else 1 for axis in range(values.ndim)]) for position in (source, target)]
    chosen = jax.random.permutation(key, shards_of)[partner]
    strong = (owner == chosen) | (owner == (partner + shards_of // 2) % shards_of)
    return jnp.where(strong, factor * values, values)


def steps_of(stream_key, extent, shards, smallest, largest):
    factor_of, own = 1.0, jax.random.fold_in(stream_key, 6)
    for axis_at, blocks in shards:
        draws = jnp.exp(jax.random.uniform(jax.random.fold_in(own, axis_at), (blocks,), jnp.float32, smallest / len(shards), largest / len(shards)))
        factor_of = factor_of * jnp.repeat(draws, extent[axis_at] // blocks).reshape([-1 if axis == axis_at else 1 for axis in range(len(extent))])
    return factor_of


def centred(rng, dims, deviation, limit, cuts=(), dtype=jnp.bfloat16):
    loudness = steps_of(rng, dims, cuts, -0.22, 0.18) if cuts else 1.0
    values = jax.random.normal(rng, dims, jnp.float32) * deviation * loudness
    return jnp.minimum(jnp.maximum(values, -limit), limit).astype(dtype)


def heavy_noise(own_key, shape, width, most, cuts, heavy, held_as=jnp.bfloat16):
    values = width * jax.random.normal(own_key, shape, jnp.float32)
    if cuts:
        values = values * steps_of(own_key, shape, cuts, -0.22, 0.18)
    return jnp.clip(spiked(values, jax.random.fold_in(own_key, 3), *heavy), -most, most).astype(held_as)


def setup_inputs(seed: int = 0) -> dict:
    streams_of = jax.random.split(jax.random.key(seed), 12)
    saved_input = heavy_noise(streams_of[0], (TOKENS, D), 1.0, 6.0, ((0, 8),), (0, 1, 8, 2.0))
    key_cotangent = centred(streams_of[1], (TOKENS, DK), ((D * TOKENS // RK) ** -0.5), 0.0625, ((0, 8), (1, 4)))
    value_cotangent = centred(streams_of[2], (TOKENS, DV), ((D * TOKENS // RV) ** -0.5), 0.0625, ((0, 8), (1, 4)))
    key_factor = centred(streams_of[3], (D, RK), RK ** -0.5, 0.375)
    value_factor = centred(streams_of[4], (D, RV), RV ** -0.5, 0.375)
    key_weight = centred(streams_of[5], (D, DK), D ** -0.5, 0.109375, ((0, 8), (1, 4)), jnp.float32)
    value_weight = centred(streams_of[6], (D, DV), D ** -0.5, 0.109375, ((0, 8), (1, 4)), jnp.float32)
    key_first = draw_key_first(jax.random.fold_in(streams_of[11], 71), 0)
    key_second = jnp.clip(jnp.exp(math.log(1.0) - 2.9957323 * jax.random.uniform(streams_of[8], (RK, DK), jnp.float32) ** steps_of(streams_of[8], (RK, DK), ((1, 4),), -0.2, 0.2)), 0.05, 1.0)
    value_first = draw_value_first(jax.random.fold_in(streams_of[11], 71), 0)
    value_second = jnp.clip(jnp.exp(math.log(1.0) - 2.9957323 * jax.random.uniform(streams_of[10], (RV, DV), jnp.float32) ** steps_of(streams_of[10], (RV, DV), ((1, 4),), -0.2, 0.2)), 0.05, 1.0)
    return dict(saved_input=saved_input, key_cotangent=key_cotangent, value_cotangent=value_cotangent, key_factor=key_factor, value_factor=value_factor, key_weight=key_weight, value_weight=value_weight, key_first=key_first, key_second=key_second, value_first=value_first, value_second=value_second)


first_decay = 0.8
second_decay = 0.9
epsilon = 1e-08
learn_rate = 0.01

def projected(saved_input, cotangent, factor):
    basis = jnp.dot(saved_input, factor, preferred_element_type=jnp.float32)
    return lax.dot_general(basis, cotangent.astype(jnp.float32), (((0,), (0,)), ((), ())), precision=lax.Precision.HIGHEST)

def moments(projection, first, second):
    first_new = first_decay * first + (1.0 - first_decay) * projection
    second_new = second_decay * second + (1.0 - second_decay) * projection * projection
    normed = first_new / (jnp.sqrt(second_new) + epsilon)
    return (first_new, second_new, normed)

def reference(saved_input, key_cotangent, value_cotangent, key_factor, value_factor, key_weight, value_weight, key_first, key_second, value_first, value_second):
    key_projected = projected(saved_input, key_cotangent, key_factor)
    value_projected = projected(saved_input, value_cotangent, value_factor)
    key_first_new, key_second_new, key_normed = moments(key_projected, key_first, key_second)
    value_first_new, value_second_new, value_normed = moments(value_projected, value_first, value_second)
    squares = jnp.sum(key_normed * key_normed) + jnp.sum(value_normed * value_normed)
    entries = jnp.float32(RK * DK + RV * DV)
    shrink = jnp.sqrt(entries / (entries + squares))
    key_step = shrink * jnp.dot(key_factor.astype(jnp.float32), key_normed, precision=lax.Precision.HIGHEST)
    value_step = shrink * jnp.dot(value_factor.astype(jnp.float32), value_normed, precision=lax.Precision.HIGHEST)
    key_weight_new = key_weight - learn_rate * key_step
    value_weight_new = value_weight - learn_rate * value_step
    return (key_weight_new, value_weight_new, key_first_new, key_second_new, value_first_new, value_second_new, key_step, value_step, key_weight_new.astype(jnp.bfloat16), value_weight_new.astype(jnp.bfloat16))
```

```python
import jax
import jax.numpy as jnp
from jax import lax
from jax.experimental import pallas as pl
from jax.experimental.pallas import tpu as pltpu
from jax.sharding import PartitionSpec as P


DK = 1024
DV = 2048
RK = 256
RV = 256


first_decay = 0.8
second_decay = 0.9
epsilon = 1e-08
learn_rate = 0.01


def split_contract(basis, cotangent):
    upper = basis.astype(jnp.bfloat16)
    lower = (basis - upper.astype(jnp.float32)).astype(jnp.bfloat16)
    dims = (((0,), (0,)), ((), ()))
    high_part = lax.dot_general(upper, cotangent, dims, preferred_element_type=jnp.float32)
    low_part = lax.dot_general(lower, cotangent, dims, preferred_element_type=jnp.float32)
    return high_part + low_part


def moments(projection, first, second):
    first_new = first_decay * first + (1.0 - first_decay) * projection
    second_new = second_decay * second + (1.0 - second_decay) * projection * projection
    normed = first_new / (jnp.sqrt(second_new) + epsilon)
    return (first_new, second_new, normed)


def body_collective(
    saved_input,
    key_cotangent,
    value_cotangent,
    key_factor,
    value_factor,
    key_weight,
    value_weight,
    key_first,
    key_second,
    value_first,
    value_second,
):
    local_rows = key_weight.shape[0]
    row_offset = lax.axis_index(("fs", "rep")) * local_rows
    key_rows = lax.dynamic_slice_in_dim(key_factor, row_offset, local_rows, 0).astype(jnp.float32)
    value_rows = lax.dynamic_slice_in_dim(value_factor, row_offset, local_rows, 0).astype(
        jnp.float32
    )
    key_basis = jnp.dot(saved_input, key_factor, preferred_element_type=jnp.float32)
    key_part = split_contract(key_basis, key_cotangent)
    value_basis = jnp.dot(saved_input, value_factor, preferred_element_type=jnp.float32)
    value_part = split_contract(value_basis, value_cotangent)
    key_projected, value_projected = lax.psum((key_part, value_part), ("fs", "rep"))
    key_first_new, key_second_new, key_normed = moments(key_projected, key_first, key_second)
    value_first_new, value_second_new, value_normed = moments(
        value_projected, value_first, value_second
    )
    local_squares = jnp.sum(key_normed * key_normed) + jnp.sum(value_normed * value_normed)
    squares = lax.psum(local_squares, "tp")
    entries = jnp.float32(RK * DK + RV * DV)
    shrink = jnp.sqrt(entries / (entries + squares))
    key_step = shrink * jnp.dot(key_rows, key_normed, precision=lax.Precision.HIGHEST)
    value_step = shrink * jnp.dot(value_rows, value_normed, precision=lax.Precision.HIGHEST)
    key_weight_new = key_weight - learn_rate * key_step
    value_weight_new = value_weight - learn_rate * value_step
    key_copy, value_copy = (
        lax.all_gather(key_weight_new.astype(jnp.bfloat16), ("fs", "rep"), axis=0, tiled=True),
        lax.all_gather(value_weight_new.astype(jnp.bfloat16), ("fs", "rep"), axis=0, tiled=True),
    )
    return (
        key_weight_new,
        value_weight_new,
        key_first_new,
        key_second_new,
        value_first_new,
        value_second_new,
        key_step,
        value_step,
        key_copy,
        value_copy,
    )


group = ("fs", "rep")
f32 = jnp.float32
bf16 = jnp.bfloat16
rep_type = bf16
fs_type = f32
back_type = f32


def shifted(value, dz, dy, fs, rep):
    perm = [
        (f * rep + r, ((f + dz) % fs) * rep + (r + dy) % rep) for f in range(fs) for r in range(rep)
    ]
    return lax.ppermute(value, group, perm)


def block_at(dz, dy, fs, rep):
    f = (lax.axis_index("fs") + dz) % fs
    r = (lax.axis_index("rep") + dy) % rep
    return (f * rep + r).astype(jnp.int32)


def halves(value):
    upper = value.astype(bf16)
    return upper, (value - upper.astype(f32)).astype(bf16)


def narrow_kernel(key_ref, value_ref, out_ref):
    width = key_ref.shape[1]
    out_ref[:, :width] = key_ref[...].astype(bf16)
    out_ref[:, width:] = value_ref[...].astype(bf16)


def project_kernel(blocks, x, key_factor, value_factor, key_cotangent, value_cotangent, *rest):
    outs, total = rest[:-1], rest[-1]
    step = pl.program_id(0)
    width = key_cotangent.shape[1]
    dims = (((0,), (0,)), ((), ()))

    @pl.when(step == 0)
    def _():
        total[...] = jnp.zeros_like(total)

    sides = (
        (key_factor, key_cotangent, slice(0, width)),
        (value_factor, value_cotangent, slice(width, total.shape[1])),
    )
    for factor, cotangent, columns in sides:
        basis = jnp.dot(x[...], factor[...], preferred_element_type=f32)
        for half in halves(basis):
            total[:, columns] += lax.dot_general(
                half, cotangent[...], dims, preferred_element_type=f32
            )

    @pl.when(step == pl.num_programs(0) - 1)
    def _():
        for place, out in enumerate(outs):
            rows = out.shape[0]
            start = pl.multiple_of(blocks[place] * rows, rows)
            out[...] = total[pl.ds(start, rows), :].astype(out.dtype)


def moments_kernel(blocks, *refs):
    stacks, refs = refs[:-11], refs[-11:]
    key_first, key_second, value_first, value_second = refs[:4]
    key_first_new, key_second_new, value_first_new, value_second_new = refs[4:8]
    upper, lower, squares = refs[8:]
    count = blocks.shape[0]
    rows = upper.shape[0] // count
    per_stack = count // len(stacks)
    width = key_first.shape[1]
    sides = (
        (key_first, key_second, key_first_new, key_second_new, slice(0, width)),
        (value_first, value_second, value_first_new, value_second_new, slice(width, upper.shape[1])),
    )
    for place in range(count):
        stack, inner = stacks[place // per_stack], place % per_stack * rows
        at = pl.ds(pl.multiple_of(blocks[place] * rows, rows), rows)
        for first, second, first_new, second_new, columns in sides:
            first_value, second_value, normed = moments(
                stack[inner : inner + rows, columns].astype(f32), first[at, :], second[at, :]
            )
            first_new[at, :] = first_value
            second_new[at, :] = second_value
            upper[at, columns], lower[at, columns] = halves(normed)
    normed = upper[...].astype(f32) + lower[...].astype(f32)
    squares[...] = jnp.full(squares.shape, jnp.sum(normed * normed), f32)


def shrink_of(entries, sums):
    squares = sums[0][0:1, 0:1]
    for other in sums[1:]:
        squares = squares + other[0:1, 0:1]
    return jnp.sqrt(entries / (entries + squares))


def step_kernel(entries, own, *refs):
    sums, refs = refs[:-10], refs[-10:]
    key_factor, value_factor, upper, lower, key_weight, value_weight = refs[:6]
    key_weight_new, value_weight_new, key_step, value_step = refs[6:]
    shrink = shrink_of(entries, sums)
    width = key_weight.shape[1]
    sides = (
        (key_factor, key_weight, key_weight_new, key_step, slice(0, width)),
        (value_factor, value_weight, value_weight_new, value_step, slice(width, upper.shape[1])),
    )
    for factor, weight, weight_new, step_out, columns in sides:
        product = jnp.dot(factor[...], upper[:, columns], preferred_element_type=f32)
        product += jnp.dot(factor[...], lower[:, columns], preferred_element_type=f32)
        product = shrink * product
        step_out[...] = product
        weight_new[...] = weight[...] - learn_rate * product


def copy_kernel(entries, *refs):
    sums, refs = refs[:-6], refs[-6:]
    key_factor, value_factor, upper, gathered, key_copy, value_copy = refs
    scale = learn_rate * shrink_of(entries, sums)
    width = key_copy.shape[1]
    for factor, copy, columns in (
        (key_factor, key_copy, slice(0, width)),
        (value_factor, value_copy, slice(width, upper.shape[1])),
    ):
        product = jnp.dot(factor[...], upper[:, columns], preferred_element_type=f32)
        copy[...] = (gathered[:, columns].astype(f32) - scale * product).astype(bf16)


def whole(shape):
    return pl.BlockSpec(shape, lambda *_: (0,) * len(shape))


def like(shape, dtype=f32):
    return jax.ShapeDtypeStruct(shape, dtype)


def body(
    saved_input,
    key_cotangent,
    value_cotangent,
    key_factor,
    value_factor,
    key_weight,
    value_weight,
    key_first,
    key_second,
    value_first,
    value_second,
):
    fs, rep, tp = lax.axis_size("fs"), lax.axis_size("rep"), lax.axis_size("tp")
    count = fs * rep
    local_rows, key_width = key_weight.shape
    value_width = value_weight.shape[1]
    width = key_width + value_width
    tokens, model = saved_input.shape
    rank = key_first.shape[0]
    piece = rank // count
    half = piece * fs
    here, row = lax.axis_index("fs"), lax.axis_index("rep")
    own = block_at(0, 0, fs, rep)
    halves_at = jnp.stack([(row + dy) % rep for dy in range(rep)]).astype(jnp.int32)
    sources = jnp.stack(
        [(row - dy) % rep * fs + (here - dz) % fs for dy in range(rep) for dz in range(fs)]
    ).astype(jnp.int32)
    weights = pl.pallas_call(
        narrow_kernel, out_shape=like((local_rows, width), bf16), name="narrow"
    )(key_weight, value_weight)
    gathered = lax.all_gather(weights, group, axis=0, tiled=True)
    parts = 1
    rows = tokens // parts
    shapes = [like((half, width))] + [like((half, width), rep_type)] * (rep - 1)
    mine, *outgoing = pl.pallas_call(
        project_kernel,
        grid_spec=pltpu.PrefetchScalarGridSpec(
            num_scalar_prefetch=1,
            grid=(parts,),
            in_specs=[
                pl.BlockSpec((rows, model), lambda i, _: (i, 0)),
                whole(key_factor.shape),
                whole(value_factor.shape),
                pl.BlockSpec((rows, key_width), lambda i, _: (i, 0)),
                pl.BlockSpec((rows, value_width), lambda i, _: (i, 0)),
            ],
            out_specs=[whole(shape.shape) for shape in shapes],
            scratch_shapes=[pltpu.VMEM((rank, width), f32)],
        ),
        out_shape=shapes,
        name="project",
    )(halves_at, saved_input, key_factor, value_factor, key_cotangent, value_cotangent)
    for dy, chunk in enumerate(outgoing, 1):
        mine = mine + shifted(chunk, 0, dy, fs, rep).astype(f32)
    cuts = [lax.dynamic_slice_in_dim(mine, (here + dz) % fs * piece, piece, 0) for dz in range(fs)]
    total = cuts[0]
    for dz in range(1, fs):
        total = total + shifted(cuts[dz].astype(fs_type), dz, 0, fs, rep).astype(f32)
    sent = total.astype(back_type)
    stack = jnp.concatenate([sent] + [shifted(sent, dz, 0, fs, rep) for dz in range(1, fs)])
    chunks = [stack] + [shifted(stack, 0, dy, fs, rep) for dy in range(1, rep)]
    results = pl.pallas_call(
        moments_kernel,
        grid_spec=pltpu.PrefetchScalarGridSpec(
            num_scalar_prefetch=1,
            grid=(1,),
            in_specs=[whole(chunk.shape) for chunk in chunks]
            + [whole((rank, key_width))] * 2
            + [whole((rank, value_width))] * 2,
            out_specs=[whole((rank, key_width))] * 2
            + [whole((rank, value_width))] * 2
            + [whole((rank, width))] * 2
            + [whole((8, 128))],
        ),
        out_shape=[like((rank, key_width))] * 2
        + [like((rank, value_width))] * 2
        + [like((rank, width), bf16)] * 2
        + [like((8, 128))],
        name="moments",
    )(sources, *chunks, key_first, key_second, value_first, value_second)
    key_first_new, key_second_new, value_first_new, value_second_new = results[:4]
    upper, lower, squares = results[4:]
    sums = [squares] + [
        lax.ppermute(squares, "tp", [(i, (i + step) % tp) for i in range(tp)])
        for step in range(1, tp)
    ]
    entries = (key_first.size + value_first.size) * tp
    block_of = lambda i, own: (own[0], 0)
    key_weight_new, value_weight_new, key_step, value_step = pl.pallas_call(
        lambda *refs: step_kernel(float(entries), *refs),
        grid_spec=pltpu.PrefetchScalarGridSpec(
            num_scalar_prefetch=1,
            grid=(1,),
            in_specs=[whole((8, 128))] * tp
            + [pl.BlockSpec((local_rows, rank), block_of)] * 2
            + [whole((rank, width))] * 2
            + [whole((local_rows, key_width)), whole((local_rows, value_width))],
            out_specs=[whole((local_rows, key_width)), whole((local_rows, value_width))] * 2,
        ),
        out_shape=[like((local_rows, key_width)), like((local_rows, value_width))] * 2,
        name="step",
    )(own[None], *sums, key_factor, value_factor, upper, lower, key_weight, value_weight)
    key_copy, value_copy = pl.pallas_call(
        lambda *refs: copy_kernel(float(entries), *refs),
        grid=(count // 2,),
        in_specs=[whole((8, 128))] * tp
        + [pl.BlockSpec((2 * local_rows, rank), lambda i: (i, 0))] * 2
        + [whole((rank, width)), pl.BlockSpec((2 * local_rows, width), lambda i: (i, 0))],
        out_specs=[
            pl.BlockSpec((2 * local_rows, key_width), lambda i: (i, 0)),
            pl.BlockSpec((2 * local_rows, value_width), lambda i: (i, 0)),
        ],
        out_shape=[like((model, key_width), bf16), like((model, value_width), bf16)],
    )(*sums, key_factor, value_factor, upper, gathered)
    return (
        key_weight_new,
        value_weight_new,
        key_first_new,
        key_second_new,
        value_first_new,
        value_second_new,
        key_step,
        value_step,
        key_copy,
        value_copy,
    )


def solution(mesh):
    in_specs = (
        P(("fs", "rep"), None),
        P(("fs", "rep"), "tp"),
        P(("fs", "rep"), "tp"),
        P(),
        P(),
        P(("fs", "rep"), "tp"),
        P(("fs", "rep"), "tp"),
        P(None, "tp"),
        P(None, "tp"),
        P(None, "tp"),
        P(None, "tp"),
    )
    out_specs = (
        P(("fs", "rep"), "tp"),
        P(("fs", "rep"), "tp"),
        P(None, "tp"),
        P(None, "tp"),
        P(None, "tp"),
        P(None, "tp"),
        P(("fs", "rep"), "tp"),
        P(("fs", "rep"), "tp"),
        P(None, "tp"),
        P(None, "tp"),
    )
    if mesh.shape["fs"] * mesh.shape["rep"] > 16:
        return jax.shard_map(
            body_collective, mesh=mesh, in_specs=in_specs, out_specs=out_specs, check_vma=False
        )
    return jax.shard_map(body, mesh=mesh, in_specs=in_specs, out_specs=out_specs, check_vma=False)
```
